32 devices in a mesh: ep: 8 (over z, y), tp: 4 (over x, core).
Axes of the slice: x: 2, y: 2, z: 4, core: 2. Of those that a mesh axis runs over, the one named last changes fastest.
Arguments:
- queries: bfloat16 [1536, 2048], P('ep', 'tp'), may hold values from -5 to 5
- keys: bfloat16 [1536, 512], P('ep', 'tp'), may hold values from -5 to 5
- values: bfloat16 [1536, 512], P('ep', 'tp'), may hold values from -6 to 6
- query_gain: float32 [128], replicated, may hold values from 0.6 to 6
- key_gain: float32 [128], replicated, may hold values from 0.6 to 6
- out_weight: bfloat16 [2048, 2048], P('tp'), may hold values from -0.125 to 0.125
- mixer_gain: float32 [2048], replicated, may hold values from 0.1 to 1.9
- expert_in: bfloat16 [4096, 2048], P(('ep', 'tp')), may hold values from -6 to 6
- routes: int32 [4096, 2], P(('ep', 'tp')), may hold values from 0 to 7, all different within a row; in each aligned block of 128 rows (0 to 127, 128 to 255, ...) at most 48 rows name the same one
- route_weights: float32 [4096, 2], P(('ep', 'tp')), may hold values from 0.2 to 1
- expert_gain: float32 [2048], replicated, may hold values from 0.5 to 4
- gate_w: bfloat16 [8, 2048, 2048], P('ep', None, 'tp'), may hold values from -0.125 to 0.125
- up_w: bfloat16 [8, 2048, 2048], P('ep', None, 'tp'), may hold values from -0.125 to 0.125
- down_w: bfloat16 [8, 2048, 2048], P('ep', 'tp'), may hold values from -0.125 to 0.125
- ffn_out_gain: float32 [2048], replicated, may hold values from 0.1 to 1.9
Outputs:
- mixer_out: bfloat16 [1536, 2048], P(('ep', 'tp'))
- expert_out: bfloat16 [4096, 2048], P(('ep', 'tp'))
The draws below stay inside these ranges and needn't reach their ends.
Inputs may be any that keep to these rules, and one draw needn't show every extreme that they name: `routes`: each row names 2 different experts. Among the rows of one device no expert is named by more than 48 rows, and in every draw some expert is named by exactly 48 rows of some device.
All inputs are finite; a program needn't handle non-finite values.
Results may differ from the reference program's by a relative error of at most 0.015.
The reference program's roundings to bfloat16 on the way count: a program that leaves them out, or rounds other values in their place, can miss the bound.
Values may be sent and summed in bfloat16 or wider, within the bound.
No kernel may reach another device: no remote copies, remote signals or barrier semaphores. Data moves between devices by JAX's collectives and lax.ppermute only.
A program may use at most 128 MiB of HBM per device.

```python
import math
import jax
import jax.numpy as jnp
import numpy as np
from jax import lax

D = 2048
HEADS = 16
KV_HEADS = 4
HEAD = 128
QW = 2048
KVW = 512
GRID_W = 64
LEN = 1536
FF = 2048
TOPK = 2
TB_DEV = 128
EXPERTS = 8
CAP = 48
TOKB = 4096
N_EP = 8
N_TP = 4


def plant_pairs(key):
    base_key = jax.random.fold_in(key, 7)
    key_part = jnp.clip(jax.random.normal(jax.random.fold_in(base_key, 1), (LEN, KVW), jnp.float32), -5.0, 5.0)
    query_part = jnp.clip(jax.random.normal(jax.random.fold_in(base_key, 2), (LEN, QW), jnp.float32), -5.0, 5.0)
    return (query_part, key_part)


def draw_queries(key, part):
    return plant_pairs(key)[0].astype(jnp.bfloat16)


def draw_keys(key, part):
    return plant_pairs(key)[1].astype(jnp.bfloat16)


def pair_gain(key, salt):
    base_key = jax.random.fold_in(key, salt)
    return jax.random.uniform(base_key, (HEAD,), jnp.float32, 0.6, 1.4)


def draw_query_gain(key, part):
    return pair_gain(key, 11)


def draw_key_gain(key, part):
    return pair_gain(key, 12)


def steps_of(key, shape, shards, least, top_value):
    def one(dim, blocks):
        heights = jax.random.uniform(jax.random.fold_in(jax.random.fold_in(key, 6), dim), (blocks,), jnp.float32, least / len(shards), top_value / len(shards))
        return jnp.repeat(jnp.exp(heights), shape[dim] // blocks).reshape((-1,) + (1,) * (len(shape) - dim - 1))

    level = one(*shards[0])
    for cut in shards[1:]:
        level = level * one(*cut)
    return level


def routed_block(stream_key, own, number, rows, number_of, top, most, slope):
    order = jax.random.permutation(stream_key, number_of)
    heavy_load, ordinary = shares(number_of, rows * top, most, slope, True), shares(number_of, rows * top, most, slope, False)
    places = jnp.arange(number_of)

    def named(tallies, turn):
        used = int((tallies > 0).sum())
        fixed = max(1, used // 4)
        shifted = fixed + (places - fixed + turn * (used - fixed)) % max(1, number_of - fixed)
        return jnp.zeros((number_of,), jnp.int32).at[order[jnp.where(places < fixed, places, shifted)]].set(jnp.asarray(tallies, jnp.int32))

    tallies = jnp.where(number % 4 == 0, named(heavy_load, number // 4), named(ordinary, number - number // 4 - 1))
    mixed = jax.random.permutation(jax.random.fold_in(own, 3), number_of)
    source_of, receiver = mixed[0:number_of // 2 * 2:2], mixed[1:number_of // 2 * 2:2]
    slack = jnp.minimum(tallies[source_of] - 1, most - tallies[receiver]) // 2
    slack = jnp.where((source_of == order[0]) | (receiver == order[0]) | (tallies[receiver] == 0), 0, jnp.maximum(slack, 0))
    shifted = jax.random.randint(jax.random.fold_in(own, 4), (number_of // 2,), 0, 1 << 20) % (slack + 1)
    tallies = tallies.at[source_of].add(-shifted).at[receiver].add(shifted)
    labels = jnp.searchsorted(jnp.cumsum(tallies), jnp.arange(rows * top), side="right").astype(jnp.int32)
    table = labels.reshape(top, rows).T
    table = table[jax.random.permutation(jax.random.fold_in(own, 1), rows)]
    turn = jax.random.randint(jax.random.fold_in(own, 2), (rows, 1), 0, top)
    return jnp.take_along_axis(table, (jnp.arange(top)[None, :] + turn) % top, axis=1)


def shares(number_of, total, most, lean, full):
    loads = [(1 << 20) // math.isqrt(standing ** lean) + 1 for standing in range(1, number_of + 1)]
    largest = most if full else min(most, max(-(-total // number_of), total * loads[0] // sum(loads)))
    least = 1 if total - largest >= number_of - 1 else 0
    given, spare = [largest] + [least] * (number_of - 1), total - largest - least * (number_of - 1)
    while spare > 0:
        movable = [i for i in range(1, number_of) if given[i] < largest] or [i for i in range(1, number_of) if given[i] < most]
        mass, left = sum([loads[i] for i in movable]), spare
        for i in movable:
            more = min(most - given[i], max(1, left * loads[i] // mass), spare)
            given[i] = given[i] + more
            spare = spare - more
    return np.array(given)


def scatter_about(key, shape, scale, reach, cuts=(), kind=jnp.bfloat16):
    entries = scale * jax.random.normal(key, shape, jnp.float32)
    if cuts:
        entries = entries * steps_of(key, shape, cuts, -0.22, 0.18)
    return jnp.clip(entries, -reach, reach).astype(kind)


def setup_inputs(seed: int = 0) -> dict:
    seeds = jax.random.split(jax.random.key(seed), 16)
    queries = draw_queries(jax.random.fold_in(seeds[15], 71), 0)
    keys = draw_keys(jax.random.fold_in(seeds[15], 71), 0)
    values = scatter_about(seeds[2], (LEN, KVW), 1.0, 6.0, ((0, 8), (1, 4)))
    query_gain = draw_query_gain(jax.random.fold_in(seeds[15], 71), 0)
    key_gain = draw_key_gain(jax.random.fold_in(seeds[15], 71), 0)
    out_weight = scatter_about(seeds[5], (QW, D), QW ** -0.5, 0.125, ((0, 4),))
    mixer_gain = jnp.clip(1.0 + 0.18 * jax.random.normal(seeds[6], (D,), jnp.float32), 0.1, 1.9)
    expert_in = scatter_about(seeds[7], (TOKB, D), 1.0, 6.0, ((0, 32),))
    routes_keys = jax.random.split(jax.random.fold_in(seeds[8], 1), TOKB // TB_DEV)
    routes_turns = jax.random.permutation(jax.random.fold_in(seeds[8], 3), TOKB // TB_DEV)
    routes = jax.vmap(lambda own, number: routed_block(jax.random.fold_in(seeds[8], 2), own, number, TB_DEV, EXPERTS, TOPK, CAP, 1))(routes_keys, routes_turns).reshape((TOKB, TOPK))
    route_weights = jnp.clip(0.2 + 0.8 * jax.random.uniform(seeds[9], (TOKB, TOPK), jnp.float32) ** steps_of(seeds[9], (TOKB, TOPK), ((0, 32),), -0.2, 0.2), 0.2, 1.0)
    expert_gain = jnp.clip(jnp.exp(jax.random.uniform(seeds[10], (D,), jnp.float32, math.log(0.5), math.log(4.0))), 0.5, 4.0)
    gate_w = scatter_about(seeds[11], (EXPERTS, D, FF), D ** -0.5, 0.125, ((0, 8), (2, 4)))
    up_w = scatter_about(seeds[12], (EXPERTS, D, FF), D ** -0.5, 0.125, ((0, 8), (2, 4)))
    down_w = scatter_about(seeds[13], (EXPERTS, FF, D), FF ** -0.5, 0.125, ((0, 8), (1, 4)))
    ffn_out_gain = jnp.clip(1.0 + 0.18 * jax.random.normal(seeds[14], (D,), jnp.float32), 0.1, 1.9)
    return {"queries": queries, "keys": keys, "values": values, "query_gain": query_gain, "key_gain": key_gain, "out_weight": out_weight, "mixer_gain": mixer_gain, "expert_in": expert_in, "routes": routes, "route_weights": route_weights, "expert_gain": expert_gain, "gate_w": gate_w, "up_w": up_w, "down_w": down_w, "ffn_out_gain": ffn_out_gain}


norm_eps = 1e-06
rope_base = 10000.0
clamp_limit = 7.0
sigmoid_slope = 1.702

def rms_scale(values_in, gain):
    return values_in * lax.rsqrt(lax.optimization_barrier(jnp.mean(values_in * values_in, axis=-1, keepdims=True)) + norm_eps) * gain

def turn_pair(halfpart, cosine, sine):
    first_part, second_part = jnp.split(halfpart, 2, axis=-1)
    return jnp.concatenate([first_part * cosine - second_part * sine, second_part * cosine + first_part * sine], axis=-1)

def grid_rotate(field, position):
    half_width = field.shape[-1] // 2
    inverse = rope_base ** (-jnp.arange(0, half_width, 2, dtype=jnp.float32) / half_width)
    grid_row = (position // GRID_W).astype(jnp.float32)
    grid_col = (position % GRID_W).astype(jnp.float32)
    row_angle = (grid_row[:, None] * inverse[None, :])[:, None, :]
    col_angle = (grid_col[:, None] * inverse[None, :])[:, None, :]
    return jnp.concatenate([turn_pair(field[..., :half_width], jnp.cos(row_angle), jnp.sin(row_angle)), turn_pair(field[..., half_width:], jnp.cos(col_angle), jnp.sin(col_angle))], axis=-1)

def clamped_unit(gate_pre, up_pre):
    gate_cut = jnp.minimum(gate_pre, clamp_limit)
    up_cut = jnp.clip(up_pre, -clamp_limit, clamp_limit)
    return ((up_cut + 1.0) * gate_cut * jax.nn.sigmoid(sigmoid_slope * gate_cut)).astype(jnp.bfloat16)

def reference(queries, keys, values, query_gain, key_gain, out_weight, mixer_gain, expert_in, routes, route_weights, expert_gain, gate_w, up_w, down_w, ffn_out_gain):
    group_size = HEADS // KV_HEADS
    position = jnp.arange(LEN, dtype=jnp.int32)
    query_norm = grid_rotate(rms_scale(queries.astype(jnp.float32).reshape(LEN, HEADS, HEAD), query_gain), position).astype(jnp.bfloat16)
    key_norm = grid_rotate(rms_scale(keys.astype(jnp.float32).reshape(LEN, KV_HEADS, HEAD), key_gain), position).astype(jnp.bfloat16)
    key_wide = key_norm.astype(jnp.float32)
    value_wide = values.reshape(LEN, KV_HEADS, HEAD).astype(jnp.float32)
    score_scale = HEAD ** (-0.5)
    query_blocks = query_norm.reshape(LEN // GRID_W, GRID_W, KV_HEADS, group_size, HEAD)

    def attend_block(block_in):
        scores = jnp.einsum('qhgd,khd->hgqk', block_in.astype(jnp.float32), key_wide) * score_scale
        expo = jnp.exp(scores - lax.optimization_barrier(jnp.max(scores, axis=-1, keepdims=True)))
        total = lax.optimization_barrier(jnp.sum(expo, axis=-1))
        probs = lax.optimization_barrier(expo.astype(jnp.bfloat16))
        summed = jnp.einsum('hgqk,khd->qhgd', probs.astype(jnp.float32), value_wide)
        return (summed / jnp.transpose(total, (2, 0, 1))[..., None]).astype(jnp.bfloat16)
    attended = lax.map(attend_block, query_blocks).reshape(LEN, HEADS * HEAD)
    column_span = HEADS * HEAD // N_TP
    projected = jnp.zeros((LEN, D), jnp.float32)
    for member in range(N_TP):
        partial_term = jnp.dot(attended[:, member * column_span:(member + 1) * column_span], out_weight[member * column_span:(member + 1) * column_span], preferred_element_type=jnp.float32).astype(jnp.bfloat16)
        projected = projected + lax.optimization_barrier(partial_term).astype(jnp.float32)
    mixer_out = rms_scale(projected, mixer_gain).astype(jnp.bfloat16)
    normed = rms_scale(expert_in.astype(jnp.float32), expert_gain).astype(jnp.bfloat16)
    padded = jnp.concatenate([normed, jnp.zeros((1, D), jnp.bfloat16)], axis=0)
    pair_expert = routes.reshape(-1)
    pair_count = pair_expert.shape[0]
    pair_weight = jnp.concatenate([route_weights.reshape(-1), jnp.zeros((1,), jnp.float32)], axis=0)
    most_rows = N_EP * N_TP * CAP
    hidden_span = FF // N_TP

    def one_expert(combined_in, expert_id):
        chosen = jnp.nonzero(pair_expert == expert_id, size=most_rows, fill_value=pair_count)[0].astype(jnp.int32)
        token_index = chosen // TOPK
        inputs = padded[token_index]
        hidden = clamped_unit(jnp.dot(inputs, gate_w[expert_id], preferred_element_type=jnp.float32), jnp.dot(inputs, up_w[expert_id], preferred_element_type=jnp.float32))
        down_here = down_w[expert_id]
        result = jnp.zeros((most_rows, D), jnp.float32)
        for member in range(N_TP):
            partial_term = jnp.dot(hidden[:, member * hidden_span:(member + 1) * hidden_span], down_here[member * hidden_span:(member + 1) * hidden_span], preferred_element_type=jnp.float32).astype(jnp.bfloat16)
            result = result + lax.optimization_barrier(partial_term).astype(jnp.float32)
        output_rows = lax.optimization_barrier(result.astype(jnp.bfloat16))
        combined_out = combined_in.at[token_index].add(pair_weight[chosen][:, None] * output_rows.astype(jnp.float32))
        return (combined_out, None)
    combined, unused = lax.scan(one_expert, jnp.zeros((TOKB + 1, D), jnp.float32), jnp.arange(EXPERTS, dtype=jnp.int32))
    expert_out = rms_scale(combined[:TOKB], ffn_out_gain).astype(jnp.bfloat16)
    return (mixer_out, expert_out)
```

```python
import jax
import jax.numpy as jnp
from jax import lax
from jax.experimental import pallas as pl
from jax.experimental.pallas import tpu as pltpu
from jax.sharding import PartitionSpec as P

HEAD = 128
GRID_W = 64


norm_eps = 1e-06
rope_base = 10000.0
clamp_limit = 7.0
sigmoid_slope = 1.702


def rms_scale(values_in, gain):
    return (
        values_in
        * lax.rsqrt(jnp.mean(values_in * values_in, axis=-1, keepdims=True) + norm_eps)
        * gain
    )


def turn_pair(halfpart, cosine, sine):
    first_part, second_part = jnp.split(halfpart, 2, axis=-1)
    return jnp.concatenate(
        [first_part * cosine - second_part * sine, second_part * cosine + first_part * sine],
        axis=-1,
    )


def grid_rotate(field, position):
    half_width = field.shape[-1] // 2
    inverse = rope_base ** (-jnp.arange(0, half_width, 2, dtype=jnp.float32) / half_width)
    grid_row = (position // GRID_W).astype(jnp.float32)
    grid_col = (position % GRID_W).astype(jnp.float32)
    row_angle = (grid_row[:, None] * inverse[None, :])[:, None, :]
    col_angle = (grid_col[:, None] * inverse[None, :])[:, None, :]
    return jnp.concatenate(
        [
            turn_pair(field[..., :half_width], jnp.cos(row_angle), jnp.sin(row_angle)),
            turn_pair(field[..., half_width:], jnp.cos(col_angle), jnp.sin(col_angle)),
        ],
        axis=-1,
    )


def clamped_unit(gate_pre, up_pre):
    gate_cut = jnp.minimum(gate_pre, clamp_limit)
    up_cut = jnp.clip(up_pre, -clamp_limit, clamp_limit)
    return ((up_cut + 1.0) * gate_cut * jax.nn.sigmoid(sigmoid_slope * gate_cut)).astype(
        jnp.bfloat16
    )


def swap(array, axis, bit):
    size = lax.axis_size(axis)
    return lax.ppermute(array, axis, [(i, i ^ bit) for i in range(size)])


def bits_of(axis):
    size = lax.axis_size(axis)
    bits = []
    bit = 1
    while bit < size:
        bits.append(bit)
        bit *= 2
    return bits


def gather_keys(packed):
    low_first = bits_of("ep")
    for bit in low_first[1:] + low_first[:1]:
        packed = jnp.concatenate([packed, swap(packed, "ep", bit)], axis=0)
    return packed


def project_shares(partial):
    size = lax.axis_size("tp")
    rows = partial.shape[0] // size
    me = lax.axis_index("tp")
    kept = partial.reshape(size, rows, partial.shape[1])
    for bit in bits_of("tp"):
        half = kept.shape[0] // 2
        pairs = kept.reshape(half, 2, rows, -1)
        upper = (me & bit) != 0
        mine = jnp.where(upper, pairs[:, 1], pairs[:, 0])
        other = jnp.where(upper, pairs[:, 0], pairs[:, 1])
        got = swap(other.astype(jnp.bfloat16), "tp", bit)
        kept = mine.astype(jnp.float32) + got.astype(jnp.float32)
    return kept[0]


def mixer_half(queries, keys, values, query_gain, key_gain, out_weight, mixer_gain):
    local_rows = queries.shape[0]
    kv_local = keys.shape[1] // HEAD
    group_size = queries.shape[1] // HEAD // kv_local
    position = lax.axis_index("ep") * local_rows + jnp.arange(local_rows, dtype=jnp.int32)
    key_f = keys.astype(jnp.float32).reshape(local_rows, kv_local, HEAD)
    key_norm = grid_rotate(rms_scale(key_f, key_gain), position).astype(jnp.bfloat16)
    key_norm = key_norm.reshape(local_rows, kv_local * HEAD)
    packed = gather_keys(jnp.concatenate([key_norm, values], axis=1))
    query_f = queries.astype(jnp.float32).reshape(local_rows, kv_local * group_size, HEAD)
    query_norm = grid_rotate(rms_scale(query_f, query_gain), position).astype(jnp.bfloat16)
    query_norm = query_norm.reshape(local_rows, kv_local, group_size, HEAD)
    score_scale = HEAD ** (-0.5)
    key_all = packed[:, : kv_local * HEAD].reshape(-1, kv_local, HEAD)
    value_all = packed[:, kv_local * HEAD :].reshape(-1, kv_local, HEAD)
    scores = (
        jnp.einsum("qhgd,khd->hgqk", query_norm, key_all, preferred_element_type=jnp.float32)
        * score_scale
    )
    expo = jnp.exp(scores - jnp.max(scores, axis=-1, keepdims=True))
    total = jnp.sum(expo, axis=-1)
    weighted = jnp.einsum(
        "hgqk,khd->hgqd", expo.astype(jnp.bfloat16), value_all, preferred_element_type=jnp.float32
    )
    attended = (weighted / total[..., None]).astype(jnp.bfloat16)
    attended = jnp.transpose(attended, (2, 0, 1, 3)).reshape(
        local_rows, kv_local * group_size * HEAD
    )
    partial = jnp.dot(attended, out_weight, preferred_element_type=jnp.float32)
    projected = project_shares(partial.astype(jnp.bfloat16))
    return rms_scale(projected, mixer_gain).astype(jnp.bfloat16)


VMEM_SPEC = pl.BlockSpec(memory_space=pltpu.VMEM)
SMEM_SPEC = pl.BlockSpec(memory_space=pltpu.SMEM)


def quarters(size):
    part = size // 4
    return [list(range(q * part, (q + 1) * part)) for q in (0, 2, 3, 1)]


def group_order(bits):
    order = [0]
    for bit in reversed(bits):
        order = order + [g | bit for g in order]
    return order


def dispatch_kernel(capacity, me_ref, rows_ref, gain_ref, turned_ref, *out_refs):
    rows = rows_ref[...].astype(jnp.float32)
    scale = lax.rsqrt(jnp.mean(rows * rows, axis=-1, keepdims=True) + norm_eps)
    normed = (rows * scale * gain_ref[...]).astype(jnp.bfloat16)
    top_count, tok_rows = turned_ref.shape
    slot_count = sum(ref.shape[0] for ref in out_refs)
    expert_count = slot_count // capacity
    relative = jnp.bitwise_xor(turned_ref[...], me_ref[0])
    expert_id = lax.broadcasted_iota(jnp.int32, (expert_count, tok_rows), 0)
    picks = [jnp.where(relative[k : k + 1] == expert_id, 1.0, 0.0) for k in range(top_count)]
    earlier = lax.broadcasted_iota(jnp.int32, (tok_rows, tok_rows), 0)
    later = lax.broadcasted_iota(jnp.int32, (tok_rows, tok_rows), 1)
    before = jnp.where(earlier < later, 1.0, 0.0).astype(jnp.bfloat16)
    ahead = jnp.dot(
        sum(picks).astype(jnp.bfloat16), before, preferred_element_type=jnp.float32
    )
    place = lax.broadcasted_iota(jnp.int32, (slot_count, tok_rows), 0)
    picked = None
    for k in range(top_count):
        rank = jnp.sum(ahead * picks[k], axis=0, keepdims=True).astype(jnp.int32)
        hit = place == relative[k : k + 1] * capacity + rank
        picked = hit if picked is None else picked | hit
    table = jnp.where(picked, 1.0, 0.0).astype(jnp.bfloat16)
    start = 0
    for ref in out_refs:
        part = table[start : start + ref.shape[0]]
        ref[...] = jnp.dot(part, normed, preferred_element_type=jnp.float32).astype(jnp.bfloat16)
        start += ref.shape[0]


def combine_kernel(capacity, me_ref, gain_ref, routes_ref, weight_ref, *refs):
    piece_refs, out_ref = refs[:-1], refs[-1]
    tok_rows, top_count = routes_ref.shape
    slot_count = sum(ref.shape[0] for ref in piece_refs)
    expert_count = slot_count // capacity
    relative = jnp.bitwise_xor(routes_ref[...], me_ref[0])
    expert_id = lax.broadcasted_iota(jnp.int32, (tok_rows, expert_count), 1)
    picks = [jnp.where(relative[:, k : k + 1] == expert_id, 1.0, 0.0) for k in range(top_count)]
    later = lax.broadcasted_iota(jnp.int32, (tok_rows, tok_rows), 0)
    earlier = lax.broadcasted_iota(jnp.int32, (tok_rows, tok_rows), 1)
    before = jnp.where(earlier < later, 1.0, 0.0).astype(jnp.bfloat16)
    ahead = jnp.dot(
        before, sum(picks).astype(jnp.bfloat16), preferred_element_type=jnp.float32
    )
    place = lax.broadcasted_iota(jnp.int32, (tok_rows, slot_count), 1)
    mixing = jnp.zeros((tok_rows, slot_count), jnp.float32)
    for k in range(top_count):
        rank = jnp.sum(ahead * picks[k], axis=1, keepdims=True).astype(jnp.int32)
        hit = place == relative[:, k : k + 1] * capacity + rank
        mixing = jnp.where(hit, weight_ref[:, k : k + 1], mixing)
    first = mixing.astype(jnp.bfloat16)
    rest = mixing - first.astype(jnp.float32)
    second = rest.astype(jnp.bfloat16)
    third = (rest - second.astype(jnp.float32)).astype(jnp.bfloat16)
    terms = jnp.concatenate([first, second, third], axis=0)
    back = jnp.concatenate([ref[...] for ref in piece_refs], axis=0)
    product = jnp.dot(terms, back, preferred_element_type=jnp.float32)
    combined = (
        product[:tok_rows] + product[tok_rows : 2 * tok_rows] + product[2 * tok_rows :]
    )
    scale = lax.rsqrt(jnp.mean(combined * combined, axis=-1, keepdims=True) + norm_eps)
    out_ref[...] = (combined * scale * gain_ref[...]).astype(jnp.bfloat16)


def expert_kernel(gate_ref, up_ref, down_ref, *refs):
    piece_refs, (keep_ref, send_ref) = refs[:-2], refs[-2:]
    rows = jnp.concatenate([ref[...] for ref in piece_refs], axis=0)
    hidden = clamped_unit(
        jnp.dot(rows, gate_ref[...], preferred_element_type=jnp.float32),
        jnp.dot(rows, up_ref[...], preferred_element_type=jnp.float32),
    )
    result = jnp.dot(hidden, down_ref[...], preferred_element_type=jnp.float32)
    half = keep_ref.shape[0]
    keep_ref[...] = result[:half].astype(jnp.bfloat16)
    send_ref[...] = result[half:].astype(jnp.bfloat16)


def run_expert(pieces, gate_local, up_local, down_local):
    bits = bits_of("tp")
    model_width = gate_local.shape[0]
    groups = {0: list(pieces)}
    for bit in reversed(bits):
        for g in list(groups):
            groups[g | bit] = [swap(piece, "tp", bit) for piece in groups[g]]
    together = [piece for g in group_order(bits) for piece in groups[g]]
    half = sum(piece.shape[0] for piece in together) // 2
    kept, sent = pl.pallas_call(
        expert_kernel,
        out_shape=[jax.ShapeDtypeStruct((half, model_width), jnp.bfloat16)] * 2,
        in_specs=[VMEM_SPEC] * (3 + len(together)),
        out_specs=[VMEM_SPEC] * 2,
        cost_estimate=pl.CostEstimate(
            flops=12 * half * model_width * gate_local.shape[1],
            bytes_accessed=8 * half * model_width,
            transcendentals=2 * half * gate_local.shape[1],
        ),
        name="expert",
    )(gate_local, up_local, down_local, *together)
    for bit in bits[1:]:
        kept = kept.astype(jnp.float32) + swap(sent, "tp", bit // 2).astype(jnp.float32)
        kept = kept.astype(jnp.bfloat16)
        half = kept.shape[0] // 2
        kept, sent = kept[:half], kept[half:]
    kept = kept.astype(jnp.float32) + swap(sent, "tp", bits[-1]).astype(jnp.float32)
    return kept.astype(jnp.bfloat16)


def expert_half(expert_in, routes, route_weights, expert_gain, gate_w, up_w, down_w, ffn_out_gain):
    tok_rows, model_width = expert_in.shape
    top_count = routes.shape[1]
    expert_count = lax.axis_size("ep")
    capacity = max(2, (3 * tok_rows * top_count + 2 * expert_count - 1) // (2 * expert_count))
    by_block = capacity % 16 == 0
    me = lax.axis_index("ep") if by_block else jnp.int32(0)
    me = me.astype(jnp.int32).reshape(1)
    block_rows = capacity if by_block else expert_count * capacity
    block_count = expert_count * capacity // block_rows
    blocks = pl.pallas_call(
        lambda *refs: dispatch_kernel(capacity, *refs),
        out_shape=[jax.ShapeDtypeStruct((block_rows, model_width), jnp.bfloat16)] * block_count,
        in_specs=[SMEM_SPEC, VMEM_SPEC, VMEM_SPEC, VMEM_SPEC],
        out_specs=[VMEM_SPEC] * block_count,
        name="dispatch",
    )(me, expert_in, expert_gain.reshape(1, -1), routes.T)
    weights = (gate_w[0], up_w[0], down_w[0])
    if by_block:
        arrived = {}
        for offsets in quarters(expert_count):
            for k in offsets:
                arrived[k] = blocks[k] if k == 0 else swap(blocks[k], "ep", k)
        returned = {}
        for offsets in quarters(expert_count):
            result = run_expert([arrived[k] for k in offsets], *weights)
            for i, k in enumerate(offsets):
                block = result[i * capacity : (i + 1) * capacity]
                returned[k] = block if k == 0 else swap(block, "ep", k)
        pieces = [returned[k] for k in range(expert_count)]
    else:
        shape = (expert_count, capacity, model_width)
        exchanged = lax.all_to_all(blocks[0].reshape(shape), "ep", 0, 0, tiled=True)
        result = run_expert([exchanged.reshape(-1, model_width)], *weights)
        pieces = [lax.all_to_all(result.reshape(shape), "ep", 0, 0, tiled=True).reshape(-1, model_width)]
    return pl.pallas_call(
        lambda *refs: combine_kernel(capacity, *refs),
        out_shape=jax.ShapeDtypeStruct((tok_rows, model_width), jnp.bfloat16),
        in_specs=[SMEM_SPEC] + [VMEM_SPEC] * (3 + len(pieces)),
        out_specs=VMEM_SPEC,
        name="combine",
    )(me, ffn_out_gain.reshape(1, -1), routes, route_weights, *pieces)


def local(
    queries,
    keys,
    values,
    query_gain,
    key_gain,
    out_weight,
    mixer_gain,
    expert_in,
    routes,
    route_weights,
    expert_gain,
    gate_w,
    up_w,
    down_w,
    ffn_out_gain,
):
    mixer_out = mixer_half(queries, keys, values, query_gain, key_gain, out_weight, mixer_gain)
    expert_out = expert_half(
        expert_in, routes, route_weights, expert_gain, gate_w, up_w, down_w, ffn_out_gain
    )
    return (mixer_out, expert_out)


def solution(mesh):
    in_specs = (
        P("ep", "tp"),
        P("ep", "tp"),
        P("ep", "tp"),
        P(),
        P(),
        P("tp", None),
        P(),
        P(("ep", "tp"), None),
        P(("ep", "tp"), None),
        P(("ep", "tp"), None),
        P(),
        P("ep", None, "tp"),
        P("ep", None, "tp"),
        P("ep", "tp", None),
        P(),
    )
    out_specs = (P(("ep", "tp"), None), P(("ep", "tp"), None))
    return jax.shard_map(local, mesh=mesh, in_specs=in_specs, out_specs=out_specs, check_vma=False)
```

```python
import functools
import math

import jax
import numpy as np
import jax.numpy as jnp
from jax import lax
from jax.experimental import pallas as pl
from jax.experimental.pallas import tpu as pltpu
from jax.sharding import PartitionSpec as P

HEAD = 128
GRID_W = 64


norm_eps = 1e-06
rope_base = 10000.0
clamp_limit = 7.0
sigmoid_slope = 1.702


def rms_scale(values_in, gain):
    return (
        values_in
        * lax.rsqrt(jnp.mean(values_in * values_in, axis=-1, keepdims=True) + norm_eps)
        * gain
    )


def clamped_unit(gate_pre, up_pre):
    gate_cut = jnp.minimum(gate_pre, clamp_limit)
    up_cut = jnp.clip(up_pre, -clamp_limit, clamp_limit)
    return ((up_cut + 1.0) * gate_cut * jax.nn.sigmoid(sigmoid_slope * gate_cut)).astype(
        jnp.bfloat16
    )


VMEM_SPEC = pl.BlockSpec(memory_space=pltpu.VMEM)
SMEM_SPEC = pl.BlockSpec(memory_space=pltpu.SMEM)


def vmem_limit(mebibytes):
    return pltpu.CompilerParams(vmem_limit_bytes=mebibytes << 20)


def swap(array, axis, bit):
    size = lax.axis_size(axis)
    return lax.ppermute(array, axis, [(i, i ^ bit) for i in range(size)])


def bits_of(axis):
    size = lax.axis_size(axis)
    bits = []
    bit = 1
    while bit < size:
        bits.append(bit)
        bit *= 2
    return bits


def quarters(size):
    part = size // 4
    return [list(range(q * part, (q + 1) * part)) for q in (0, 2, 3, 1)]


def group_order(bits):
    order = [0]
    for bit in reversed(bits):
        order = order + [g | bit for g in order]
    return order


def merge_kernel(kept_ref, got_ref, *out_refs):
    start = 0
    for ref in out_refs:
        rows = slice(start, start + ref.shape[0])
        total = kept_ref[rows].astype(jnp.float32) + got_ref[rows].astype(jnp.float32)
        ref[...] = total.astype(jnp.bfloat16)
        start += ref.shape[0]


def finish_kernel(gain_ref, kept_ref, got_ref, out_ref):
    total = kept_ref[...].astype(jnp.float32) + got_ref[...].astype(jnp.float32)
    out_ref[...] = rms_scale(total, gain_ref[...]).astype(jnp.bfloat16)


def stack_kernel(axis, first_ref, second_ref, out_ref):
    out_ref[...] = jnp.concatenate([first_ref[...], second_ref[...]], axis=axis)


def small_call(kernel, shapes, *operands):
    out_shape = [jax.ShapeDtypeStruct(shape, jnp.bfloat16) for shape in shapes]
    held = sum(2 * math.prod(shape) for shape in shapes)
    return pl.pallas_call(
        kernel,
        out_shape=out_shape,
        in_specs=[VMEM_SPEC] * len(operands),
        out_specs=[VMEM_SPEC] * len(shapes),
        compiler_params=vmem_limit(3 + held // (1 << 18)),
    )(*operands)


def stack(first, second, axis):
    shape = list(first.shape)
    shape[axis] += second.shape[axis]
    return small_call(functools.partial(stack_kernel, axis), [tuple(shape)], first, second)[0]


def reduce_shares(kept, sent, bits):
    width = kept.shape[1]
    for bit in bits[:-1]:
        got = swap(sent, "tp", bit)
        half = kept.shape[0] // 2
        kept, sent = small_call(merge_kernel, [(half, width)] * 2, kept, got)
    return kept, swap(sent, "tp", bits[-1])


def load_kernel(*refs):
    count = len(refs) // 3
    sources, targets, semaphores = refs[:count], refs[count : 2 * count], refs[2 * count :]
    copies = [
        pltpu.make_async_copy(source, target, semaphore)
        for source, target, semaphore in zip(sources, targets, semaphores)
    ]
    for copy in copies:
        copy.start()
    for copy in copies:
        copy.wait()


def load(arrays):
    return pl.pallas_call(
        load_kernel,
        out_shape=[pltpu.VMEM(array.shape, array.dtype) for array in arrays],
        in_specs=[pl.BlockSpec(memory_space=pl.ANY)] * len(arrays),
        out_specs=[VMEM_SPEC] * len(arrays),
        scratch_shapes=[pltpu.SemaphoreType.DMA] * len(arrays),
        compiler_params=vmem_limit(2),
        name="load",
    )(*arrays)


def rotation_table(count):
    quarter = HEAD // 4
    power = -np.arange(0, HEAD // 2, 2, dtype=np.float32) / np.float32(HEAD // 2)
    inverse = np.power(np.float32(rope_base), power).astype(np.float32)
    angle = np.arange(count, dtype=np.float32)[:, None] * np.tile(inverse, 4)[None, :]
    sign = np.where(np.arange(HEAD) % (2 * quarter) < quarter, -1.0, 1.0)
    wide = angle.astype(np.float64)
    return np.concatenate([np.cos(wide), np.sin(wide) * sign], axis=1).astype(np.float32)


def norm_rotate(field, gain, cosine, sine):
    quarter = HEAD // 4
    field = field.astype(jnp.float32)
    scale = lax.rsqrt(jnp.mean(field * field, axis=-1, keepdims=True) + norm_eps)
    field = field * scale * gain
    lane = lax.broadcasted_iota(jnp.int32, field.shape, 1)
    partner = jnp.where(
        lane % (2 * quarter) < quarter,
        pltpu.roll(field, HEAD - quarter, 1),
        pltpu.roll(field, quarter, 1),
    )
    return (field * cosine + partner * sine).astype(jnp.bfloat16)


def attention_kernel(
    order,
    key_bits,
    me_ref,
    queries_ref,
    query_gain_ref,
    key_gain_ref,
    row_table_ref,
    column_table_ref,
    packed_ref,
    weight_ref,
    keep_ref,
    send_ref,
    turned_ref,
    cosine_ref,
    sine_ref,
):
    share = queries_ref.shape[0] // len(order)
    starts = [pl.multiple_of(jnp.bitwise_xor(me_ref[1], g) * share, share) for g in order]
    heads = queries_ref.shape[1] // HEAD
    key_rows = packed_ref.shape[0]
    kv_heads = packed_ref.shape[1] // HEAD // 2
    block = max(size for size in range(1, min(key_rows, 2048) + 1) if key_rows % size == 0)
    score_scale = HEAD ** (-0.5)

    def tables_of(grid_row):
        by_row = jnp.broadcast_to(row_table_ref[pl.ds(grid_row, 1)], column_table_ref.shape)
        lane = lax.broadcasted_iota(jnp.int32, by_row.shape, 1)
        both = jnp.where(lane % HEAD < HEAD // 2, by_row, column_table_ref[...])
        return both[:, :HEAD], both[:, HEAD:]

    local_rows = queries_ref.shape[0]
    grid_rows = local_rows // GRID_W

    def turn_keys(shard, offset):
        owner = jnp.bitwise_xor(me_ref[0], offset)
        for i in range(grid_rows):
            start_row = shard * local_rows + i * GRID_W
            rows = pl.ds(pl.multiple_of(start_row, GRID_W), GRID_W)
            cosine, sine = tables_of(owner * grid_rows + i)
            for start in range(0, kv_heads * HEAD, HEAD):
                columns = slice(start, start + HEAD)
                turned_ref[rows, columns] = norm_rotate(
                    packed_ref[rows, columns], key_gain_ref[...], cosine, sine
                )

    def one_shard(shard, unused):
        offset = jnp.int32(0)
        for place, bit in enumerate(key_bits):
            offset = offset | (((shard >> place) & 1) * bit)
        turn_keys(shard, offset)
        return unused

    lax.fori_loop(0, key_rows // local_rows, one_shard, 0)
    for i in range(grid_rows):
        rows = slice(i * GRID_W, (i + 1) * GRID_W)
        cosine_ref[rows], sine_ref[rows] = tables_of(me_ref[0] * grid_rows + i)
    cosine = jnp.concatenate([cosine_ref[pl.ds(start, share)] for start in starts], axis=0)
    sine = jnp.concatenate([sine_ref[pl.ds(start, share)] for start in starts], axis=0)
    finished = []
    for head in range(heads):
        columns = slice(head * HEAD, (head + 1) * HEAD)
        query = jnp.concatenate([queries_ref[pl.ds(start, share), columns] for start in starts], axis=0)
        query = norm_rotate(query, query_gain_ref[...], cosine, sine)
        kv_head = head // (heads // kv_heads)
        key_columns = slice(kv_head * HEAD, (kv_head + 1) * HEAD)
        value_columns = slice((kv_heads + kv_head) * HEAD, (kv_heads + kv_head + 1) * HEAD)

        def scores_of(rows):
            return score_scale * lax.dot_general(
                query,
                turned_ref[rows, key_columns],
                (((1,), (1,)), ((), ())),
                preferred_element_type=jnp.float32,
            )

        def weigh(scores, top, rows):
            expo = jnp.exp(scores - top)
            weighted = jnp.dot(
                expo.astype(jnp.bfloat16),
                packed_ref[rows, value_columns],
                preferred_element_type=jnp.float32,
            )
            return jnp.sum(expo, axis=-1, keepdims=True), weighted

        if block == key_rows:
            scores = scores_of(slice(None))
            total, weighted = weigh(scores, jnp.max(scores, axis=-1, keepdims=True), slice(None))
        else:

            def one_block(i, state):
                top, total, weighted = state
                rows = pl.ds(pl.multiple_of(i * block, block), block)
                scores = scores_of(rows)
                new_top = jnp.maximum(top, jnp.max(scores, axis=-1, keepdims=True))
                factor = jnp.exp(top - new_top)
                more_total, more_weighted = weigh(scores, new_top, rows)
                return (new_top, total * factor + more_total, weighted * factor + more_weighted)

            query_rows = query.shape[0]
            _, total, weighted = lax.fori_loop(
                0,
                key_rows // block,
                one_block,
                (
                    jnp.full((query_rows, 1), -1e30, jnp.float32),
                    jnp.zeros((query_rows, 1), jnp.float32),
                    jnp.zeros((query_rows, HEAD), jnp.float32),
                ),
            )
        finished.append((weighted / total).astype(jnp.bfloat16))
    attended = jnp.concatenate(finished, axis=1)
    partial = jnp.dot(attended, weight_ref[...], preferred_element_type=jnp.float32)
    half = keep_ref.shape[0]
    keep_ref[...] = partial[:half].astype(jnp.bfloat16)
    send_ref[...] = partial[half:].astype(jnp.bfloat16)


def mixer_half(me, queries, keys, values, query_gain, key_gain, out_weight, mixer_gain):
    local_rows = queries.shape[0]
    model_width = out_weight.shape[1]
    packed = stack(keys, values, 1)
    low_first = bits_of("ep")
    key_bits = low_first[1:] + low_first[:1]
    for bit in key_bits:
        packed = stack(packed, swap(packed, "ep", bit), 0)
    row_table = rotation_table(packed.shape[0] // GRID_W)
    column_table = rotation_table(GRID_W)
    bits = bits_of("tp")
    order = group_order(bits)
    kept, sent = pl.pallas_call(
        lambda *refs: attention_kernel(order, key_bits, *refs),
        out_shape=[jax.ShapeDtypeStruct((local_rows // 2, model_width), jnp.bfloat16)] * 2,
        in_specs=[SMEM_SPEC] + [VMEM_SPEC] * 7,
        out_specs=[VMEM_SPEC] * 2,
        scratch_shapes=[
            pltpu.VMEM((packed.shape[0], keys.shape[1]), jnp.bfloat16),
            pltpu.VMEM((local_rows, HEAD), jnp.float32),
            pltpu.VMEM((local_rows, HEAD), jnp.float32),
        ],
        compiler_params=vmem_limit(12 + packed.shape[0] // 1024),
        name="attention",
    )(
        me,
        queries,
        query_gain.reshape(1, -1),
        key_gain.reshape(1, -1),
        row_table,
        column_table,
        packed,
        out_weight,
    )
    kept, got = reduce_shares(kept, sent, bits)
    return small_call(finish_kernel, [kept.shape], mixer_gain.reshape(1, -1), kept, got)[0]


def dispatch_kernel(capacity, me_ref, rows_ref, gain_ref, turned_ref, *out_refs):
    rows = rows_ref[...].astype(jnp.float32)
    scale = lax.rsqrt(jnp.mean(rows * rows, axis=-1, keepdims=True) + norm_eps)
    normed = (rows * scale * gain_ref[...]).astype(jnp.bfloat16)
    top_count, tok_rows = turned_ref.shape
    slot_count = sum(ref.shape[0] for ref in out_refs)
    expert_count = slot_count // capacity
    relative = jnp.bitwise_xor(turned_ref[...], me_ref[0])
    expert_id = lax.broadcasted_iota(jnp.int32, (expert_count, tok_rows), 0)
    picks = [jnp.where(relative[k : k + 1] == expert_id, 1.0, 0.0) for k in range(top_count)]
    earlier = lax.broadcasted_iota(jnp.int32, (tok_rows, tok_rows), 0)
    later = lax.broadcasted_iota(jnp.int32, (tok_rows, tok_rows), 1)
    before = jnp.where(earlier < later, 1.0, 0.0).astype(jnp.bfloat16)
    ahead = jnp.dot(
        sum(picks).astype(jnp.bfloat16), before, preferred_element_type=jnp.float32
    )
    place = lax.broadcasted_iota(jnp.int32, (slot_count, tok_rows), 0)
    picked = None
    for k in range(top_count):
        rank = jnp.sum(ahead * picks[k], axis=0, keepdims=True).astype(jnp.int32)
        hit = place == relative[k : k + 1] * capacity + rank
        picked = hit if picked is None else picked | hit
    table = jnp.where(picked, 1.0, 0.0).astype(jnp.bfloat16)
    start = 0
    for ref in out_refs:
        part = table[start : start + ref.shape[0]]
        ref[...] = jnp.dot(part, normed, preferred_element_type=jnp.float32).astype(jnp.bfloat16)
        start += ref.shape[0]


def combine_kernel(capacity, me_ref, gain_ref, routes_ref, weight_ref, *refs):
    piece_refs, out_ref = refs[:-1], refs[-1]
    tok_rows, top_count = routes_ref.shape
    slot_count = sum(ref.shape[0] for ref in piece_refs)
    expert_count = slot_count // capacity
    relative = jnp.bitwise_xor(routes_ref[...], me_ref[0])
    expert_id = lax.broadcasted_iota(jnp.int32, (tok_rows, expert_count), 1)
    picks = [jnp.where(relative[:, k : k + 1] == expert_id, 1.0, 0.0) for k in range(top_count)]
    later = lax.broadcasted_iota(jnp.int32, (tok_rows, tok_rows), 0)
    earlier = lax.broadcasted_iota(jnp.int32, (tok_rows, tok_rows), 1)
    before = jnp.where(earlier < later, 1.0, 0.0).astype(jnp.bfloat16)
    ahead = jnp.dot(
        before, sum(picks).astype(jnp.bfloat16), preferred_element_type=jnp.float32
    )
    place = lax.broadcasted_iota(jnp.int32, (tok_rows, slot_count), 1)
    mixing = jnp.zeros((tok_rows, slot_count), jnp.float32)
    for k in range(top_count):
        rank = jnp.sum(ahead * picks[k], axis=1, keepdims=True).astype(jnp.int32)
        hit = place == relative[:, k : k + 1] * capacity + rank
        mixing = jnp.where(hit, weight_ref[:, k : k + 1], mixing)
    first = mixing.astype(jnp.bfloat16)
    rest = mixing - first.astype(jnp.float32)
    second = rest.astype(jnp.bfloat16)
    third = (rest - second.astype(jnp.float32)).astype(jnp.bfloat16)
    terms = jnp.concatenate([first, second, third], axis=0)
    back = jnp.concatenate([ref[...] for ref in piece_refs], axis=0)
    product = jnp.dot(terms, back, preferred_element_type=jnp.float32)
    combined = (
        product[:tok_rows] + product[tok_rows : 2 * tok_rows] + product[2 * tok_rows :]
    )
    scale = lax.rsqrt(jnp.mean(combined * combined, axis=-1, keepdims=True) + norm_eps)
    out_ref[...] = (combined * scale * gain_ref[...]).astype(jnp.bfloat16)


def expert_kernel(gate_ref, up_ref, down_ref, *refs):
    piece_refs, (keep_ref, send_ref) = refs[:-2], refs[-2:]
    rows = jnp.concatenate([ref[...] for ref in piece_refs], axis=0)
    hidden = clamped_unit(
        jnp.dot(rows, gate_ref[...], preferred_element_type=jnp.float32),
        jnp.dot(rows, up_ref[...], preferred_element_type=jnp.float32),
    )
    result = jnp.dot(hidden, down_ref[...], preferred_element_type=jnp.float32)
    half = keep_ref.shape[0]
    keep_ref[...] = result[:half].astype(jnp.bfloat16)
    send_ref[...] = result[half:].astype(jnp.bfloat16)


def run_expert(named_pieces, gate_local, up_local, down_local):
    bits = bits_of("tp")
    model_width = gate_local.shape[0]
    groups = {0: named_pieces}
    for bit in reversed(bits):
        for g in list(groups):
            groups[g | bit] = [(name, swap(piece, "tp", bit)) for name, piece in groups[g]]
    together = [piece for g in group_order(bits) for _, piece in groups[g]]
    half = sum(piece.shape[0] for piece in together) // 2
    kept, sent = pl.pallas_call(
        expert_kernel,
        out_shape=[jax.ShapeDtypeStruct((half, model_width), jnp.bfloat16)] * 2,
        in_specs=[VMEM_SPEC] * (3 + len(together)),
        out_specs=[VMEM_SPEC] * 2,
        compiler_params=vmem_limit(17),
        name="expert",
    )(gate_local, up_local, down_local, *together)
    kept, got = reduce_shares(kept, sent, bits)
    shapes = [piece.shape for _, piece in named_pieces]
    return small_call(merge_kernel, shapes, kept, got)


def expert_half(
    me, expert_in, routes, route_weights, expert_gain, gate_w, up_w, down_w, ffn_out_gain
):
    tok_rows, model_width = expert_in.shape
    top_count = routes.shape[1]
    expert_count = lax.axis_size("ep")
    capacity = max(2, (3 * tok_rows * top_count + 2 * expert_count - 1) // (2 * expert_count))
    by_block = capacity % 16 == 0
    if not by_block:
        me = jnp.zeros_like(me)
    block_rows = capacity if by_block else expert_count * capacity
    block_count = expert_count * capacity // block_rows
    blocks = pl.pallas_call(
        lambda *refs: dispatch_kernel(capacity, *refs),
        out_shape=[jax.ShapeDtypeStruct((block_rows, model_width), jnp.bfloat16)] * block_count,
        in_specs=[SMEM_SPEC, VMEM_SPEC, VMEM_SPEC, VMEM_SPEC],
        out_specs=[VMEM_SPEC] * block_count,
        compiler_params=vmem_limit(6),
        name="dispatch",
    )(me, expert_in, expert_gain.reshape(1, -1), routes.T)
    weights = load((gate_w[0], up_w[0], down_w[0]))
    if by_block:
        arrived, returned = {0: blocks[0]}, {}
        for k in range(1, expert_count):
            arrived[k] = swap(blocks[k], "ep", k)
        for offsets in quarters(expert_count):
            results = run_expert([(k, arrived[k]) for k in offsets], *weights)
            for k, block in zip(offsets, results):
                returned[k] = block if k == 0 else swap(block, "ep", k)
        pieces = [returned[k] for k in range(expert_count)]
    else:
        shape = (expert_count, capacity, model_width)
        exchanged = lax.all_to_all(blocks[0].reshape(shape), "ep", 0, 0, tiled=True)
        result = run_expert([(0, exchanged.reshape(-1, model_width))], *weights)[0]
        back = lax.all_to_all(result.reshape(shape), "ep", 0, 0, tiled=True)
        pieces = [back.reshape(-1, model_width)]
    return pl.pallas_call(
        lambda *refs: combine_kernel(capacity, *refs),
        out_shape=jax.ShapeDtypeStruct((tok_rows, model_width), jnp.bfloat16),
        in_specs=[SMEM_SPEC] + [VMEM_SPEC] * (3 + len(pieces)),
        out_specs=VMEM_SPEC,
        compiler_params=vmem_limit(9),
        name="combine",
    )(me, ffn_out_gain.reshape(1, -1), routes, route_weights, *pieces)


def local(
    queries,
    keys,
    values,
    query_gain,
    key_gain,
    out_weight,
    mixer_gain,
    expert_in,
    routes,
    route_weights,
    expert_gain,
    gate_w,
    up_w,
    down_w,
    ffn_out_gain,
):
    me = jnp.stack([lax.axis_index("ep"), lax.axis_index("tp")]).astype(jnp.int32)
    mixer_out = mixer_half(me, queries, keys, values, query_gain, key_gain, out_weight, mixer_gain)
    expert_out = expert_half(
        me, expert_in, routes, route_weights, expert_gain, gate_w, up_w, down_w, ffn_out_gain
    )
    return (mixer_out, expert_out)


def solution(mesh):
    in_specs = (
        P("ep", "tp"),
        P("ep", "tp"),
        P("ep", "tp"),
        P(),
        P(),
        P("tp", None),
        P(),
        P(("ep", "tp"), None),
        P(("ep", "tp"), None),
        P(("ep", "tp"), None),
        P(),
        P("ep", None, "tp"),
        P("ep", None, "tp"),
        P("ep", "tp", None),
        P(),
    )
    out_specs = (P(("ep", "tp"), None), P(("ep", "tp"), None))
    return jax.shard_map(local, mesh=mesh, in_specs=in_specs, out_specs=out_specs, check_vma=False)
```
